32 devices in a mesh: dp: 2 (over x), kv: 8 (over z, y), tp: 2 (over core).
Axes of the slice: x: 2, y: 2, z: 4, core: 2. Of those that a mesh axis runs over, the one named last changes fastest.
Arguments:
- tokens: bfloat16 [32, 16, 4096], P('dp', None, 'kv'), may hold values from -64 to 64
- in_gain: bfloat16 [4096], P('kv'), may hold values from 0.099609375 to 1.8984375
- query_weight: bfloat16 [4096, 4096], P('kv', 'tp'), may hold values from -0.125 to 0.125
- key_weight: bfloat16 [4096, 4096], P('kv', 'tp'), may hold values from -0.125 to 0.125
- value_weight: bfloat16 [4096, 4096], P('kv', 'tp'), may hold values from -0.09375 to 0.09375
- out_weight: bfloat16 [4096, 4096], P('tp', 'kv'), may hold values from -0.1875 to 0.1875
- lambdas: float32 [16], P('tp'), may hold values from 0.3 to 0.8
- sub_gain: bfloat16 [256], replicated, may hold values from 0.099609375 to 1.8984375
- key_cache: bfloat16 [32, 256, 16, 2, 128], P('dp', 'kv', 'tp'), may hold values from -248 to 248
- value_cache: bfloat16 [32, 256, 16, 256], P('dp', 'kv', 'tp'), may hold values from -6 to 6
- cache_len: int32 [32], P('dp'), may hold values from 128 to 224
- accepted: int32 [32], P('dp'), may hold values from 0 to 16
- parents: int32 [32, 16], P('dp'), may hold values from -1 to 14, as said below
Outputs:
- output: bfloat16 [32, 16, 4096], P('dp', None, ('kv', 'tp'))
- key_cache_out: bfloat16 [32, 256, 16, 2, 128], P('dp', 'kv', 'tp')
- value_cache_out: bfloat16 [32, 256, 16, 256], P('dp', 'kv', 'tp')
The draws below stay inside these ranges and needn't reach their ends.
Inputs may be any that keep to these rules, and one draw needn't show every extreme that they name: `parents`: each proposal's parent is -1 (the text already in the cache) or one of the three proposals just before it; the last proposal's parent is the one just before it. Positions below cache_len plus accepted hold a sequence's text; the later ones are stale.
All inputs are finite; a program needn't handle non-finite values.
Results may differ from the reference program's by a relative error of at most 0.019.
The reference program's roundings to bfloat16 on the way count: a program that leaves them out, or rounds other values in their place, can miss the bound.
Values may be sent and summed in bfloat16 or wider, within the bound.
No kernel may reach another device: no remote copies, remote signals or barrier semaphores. Data moves between devices by JAX's collectives and lax.ppermute only.
A program may use at most 64 MiB of HBM per device.

```python
import math
import jax
import jax.numpy as jnp
from jax import lax

D = 4096
HD = 128
H = 16
P_SIZE = 16
POS_DEV = 32
BATCH = 32
LEN = 256
N_TP = 2


def draw_tokens(key, part):
    key_one = jax.random.fold_in(key, 0)
    column = 10.0 ** (jnp.arange(D, dtype=jnp.float32) / D)
    values = jax.random.normal(key_one, (BATCH, P_SIZE, D), jnp.float32) * column
    return jnp.clip(values, -64.0, 64.0).astype(jnp.bfloat16)


def draw_key_cache(key, part):
    key_one = jax.random.fold_in(key, 0)
    noise = jnp.clip(jax.random.normal(key_one, (BATCH, LEN, H, 2, HD), jnp.float32) * 1.3, -8.0, 8.0)
    return noise.astype(jnp.bfloat16)


def draw_parents(key, part):
    step_back = jax.random.randint(key, (BATCH, P_SIZE), 0, 3)
    last_column = (jnp.arange(P_SIZE, dtype=jnp.int32) == P_SIZE - 1)[None, :]
    step_back = jnp.where(last_column, 0, step_back)
    return jnp.maximum(jnp.arange(P_SIZE, dtype=jnp.int32)[None, :] - 1 - step_back, -1).astype(jnp.int32)


def place_ends(result, own_key, least, largest):
    longest = result.shape.index(max(result.shape))
    spots = []
    for shift in (0, 1):
        where = [jax.random.randint(jax.random.fold_in(own_key, axis), (), 0, length) for axis, length in enumerate(result.shape)]
        where[longest] = (where[longest] + shift) % result.shape[longest]
        spots.append(tuple(where))
    return result.at[spots[0]].set(least).at[spots[1]].set(largest)


def levels(stream_key, extent, shards, smallest, high):
    def one(position, blocks):
        draws = jax.random.uniform(jax.random.fold_in(jax.random.fold_in(stream_key, 6), position), (blocks,), jnp.float32, smallest / len(shards), high / len(shards))
        return jnp.repeat(jnp.exp(draws), extent[position] // blocks).reshape((-1,) + (1,) * (len(extent) - position - 1))

    loudness = one(*shards[0])
    for cut in shards[1:]:
        loudness = loudness * one(*cut)
    return loudness


def gaussian(key, dims, deviation, most, pieces=(), kind=jnp.bfloat16):
    values = deviation * jax.random.normal(key, dims, jnp.float32)
    if pieces:
        values = values * levels(key, dims, pieces, -0.22, 0.18)
    return jnp.clip(values, -most, most).astype(kind)


def setup_inputs(seed: int = 0) -> dict:
    key_list = jax.random.split(jax.random.key(seed), 14)
    return {
        "tokens": draw_tokens(jax.random.fold_in(key_list[13], 71), 0),
        "in_gain": jnp.clip(1.0 + 0.18 * jax.random.normal(key_list[1], (D,), jnp.float32), 0.099609375, 1.8984375).astype(jnp.bfloat16),
        "query_weight": gaussian(key_list[2], (D, D), (D * 10 // 17) ** -0.5, 0.125, ((0, 8), (1, 2))),
        "key_weight": gaussian(key_list[3], (D, D), (D * 10 // 17) ** -0.5, 0.125, ((0, 8), (1, 2))),
        "value_weight": gaussian(key_list[4], (D, D), D ** -0.5, 0.09375, ((0, 8), (1, 2))),
        "out_weight": gaussian(key_list[5], (D, D), (D // 4) ** -0.5, 0.1875, ((0, 2), (1, 8))),
        "lambdas": jnp.clip(0.3 + 0.5 * jax.random.uniform(key_list[6], (H,), jnp.float32) ** levels(key_list[6], (H,), ((0, 2),), -0.2, 0.2), 0.3, 0.8),
        "sub_gain": jnp.clip(1.0 + 0.18 * jax.random.normal(key_list[7], (2 * HD,), jnp.float32), 0.099609375, 1.8984375).astype(jnp.bfloat16),
        "key_cache": draw_key_cache(jax.random.fold_in(key_list[13], 71), 0),
        "value_cache": gaussian(key_list[9], (BATCH, LEN, H, 2 * HD), 1.0, 6.0, ((0, 2), (1, 8), (2, 2))),
        "cache_len": place_ends(jax.random.randint(key_list[10], (BATCH,), LEN // 2, LEN - 2 * P_SIZE + 1), jax.random.fold_in(key_list[10], 1), LEN // 2, LEN - 2 * P_SIZE).astype(jnp.int32),
        "accepted": place_ends(jax.random.randint(key_list[11], (BATCH,), 0, P_SIZE + 1), jax.random.fold_in(key_list[11], 1), 0, P_SIZE).astype(jnp.int32),
        "parents": draw_parents(jax.random.fold_in(key_list[13], 71), 0),
    }


LAMBDA_SCALE = 0.2 + 0.6 * math.exp(-0.6)
NEG_FILL = -1e+30

def visible_links(parents):
    number = parents.shape[-1]
    identity = jnp.eye(number, dtype=jnp.float32)
    parent_links = (parents[..., :, None] == jnp.arange(number, dtype=jnp.int32)[None, :]).astype(jnp.float32)

    def extend(repeat, reached):
        return jnp.maximum(identity, jnp.einsum('bij,bjk->bik', parent_links, reached, precision=lax.Precision.HIGHEST))
    reached = lax.fori_loop(0, number, extend, jnp.broadcast_to(identity, parent_links.shape))
    depths = (lax.optimization_barrier(jnp.sum(reached, axis=-1)) - 1.0).astype(jnp.int32)
    return (reached > 0.5, depths)

def rotate(values, positions):
    half_dim = values.shape[-1] // 2
    frequency = 10000.0 ** (-jnp.arange(half_dim, dtype=jnp.float32) / half_dim)
    angles = positions.astype(jnp.float32)[..., None] * frequency
    cosine = jnp.cos(angles)[..., None, None, :]
    sine_part = jnp.sin(angles)[..., None, None, :]
    lower_half = values[..., :half_dim]
    upper_half = values[..., half_dim:]
    return jnp.concatenate([lower_half * cosine - upper_half * sine_part, upper_half * cosine + lower_half * sine_part], axis=-1)

def reference(tokens, in_gain, query_weight, key_weight, value_weight, out_weight, lambdas, sub_gain, key_cache, value_cache, cache_len, accepted, parents):
    batch_size, prop_count, width_all = tokens.shape
    head_count = lambdas.shape[0]
    head_dim = key_cache.shape[-1]
    tokens_wide = tokens.astype(jnp.float32)
    squares = lax.optimization_barrier(jnp.sum(tokens_wide * tokens_wide, axis=-1))
    row_scale = lax.rsqrt(squares / width_all + 1e-06)[..., None]
    normed = (tokens_wide * in_gain.astype(jnp.float32)).astype(jnp.bfloat16).reshape(batch_size * prop_count, width_all)
    starts = cache_len + accepted
    visible, depths = visible_links(parents)
    positions = starts[:, None] + depths

    def project(weight):
        product = jnp.dot(normed, weight, preferred_element_type=jnp.float32)
        return product.reshape(batch_size, prop_count, -1) * row_scale
    vec_shape = (batch_size, prop_count, head_count, 2, head_dim)
    queries = rotate(project(query_weight).reshape(vec_shape), positions).astype(jnp.bfloat16)
    new_keys = rotate(project(key_weight).reshape(vec_shape), positions).astype(jnp.bfloat16)
    new_values = project(value_weight).reshape(batch_size, prop_count, head_count, 2 * head_dim).astype(jnp.bfloat16)
    slot_index = starts[:, None] + jnp.arange(prop_count, dtype=jnp.int32)[None, :]
    seq_index = jnp.broadcast_to(jnp.arange(batch_size, dtype=jnp.int32)[:, None], slot_index.shape)
    key_out = key_cache.at[seq_index, slot_index].set(new_keys)
    value_out = value_cache.at[seq_index, slot_index].set(new_values)
    lam_mix = lambdas[:, None, None]
    inverse_root = head_dim ** (-0.5)

    def one_sequence(sequence_items):
        query_rows, key_new, value_new, key_rows, value_rows, start_pos, seen_mask = sequence_items
        length = key_rows.shape[0]
        query_wide = query_rows.astype(jnp.float32)
        cache_scores = jnp.einsum('qhmd,thmd->hmqt', query_wide, key_rows.astype(jnp.float32)) * inverse_root
        live_mask = (jnp.arange(length, dtype=jnp.int32) < start_pos)[None, None, None, :]
        cache_scores = jnp.where(live_mask, cache_scores, NEG_FILL)
        own_scores = jnp.einsum('qhmd,jhmd->hmqj', query_wide, key_new.astype(jnp.float32)) * inverse_root
        own_mask = seen_mask[None, None]
        own_scores = jnp.where(own_mask, own_scores, NEG_FILL)
        highest = jnp.maximum(lax.optimization_barrier(jnp.max(cache_scores, axis=-1)), lax.optimization_barrier(jnp.max(own_scores, axis=-1)))
        cache_exp = jnp.where(live_mask, jnp.exp(cache_scores - highest[..., None]), 0.0)
        own_exp = jnp.where(own_mask, jnp.exp(own_scores - highest[..., None]), 0.0)
        totals = lax.optimization_barrier(jnp.sum(cache_exp, axis=-1)) + lax.optimization_barrier(jnp.sum(own_exp, axis=-1))
        cache_prob = cache_exp / totals[..., None]
        own_prob = own_exp / totals[..., None]
        cache_weight = (cache_prob[:, 0] - lam_mix * cache_prob[:, 1]).astype(jnp.bfloat16)
        own_weight = (own_prob[:, 0] - lam_mix * own_prob[:, 1]).astype(jnp.bfloat16)
        blocks = length // POS_DEV
        block_weight = cache_weight.reshape(head_count, prop_count, blocks, POS_DEV).astype(jnp.float32)
        block_values = value_rows.reshape(blocks, POS_DEV, head_count, 2 * head_dim).astype(jnp.float32)
        partial_value = jnp.einsum('hqnt,nthe->nqhe', block_weight, block_values)
        partial_value = lax.optimization_barrier(partial_value.astype(jnp.bfloat16)).astype(jnp.float32)
        own_term = jnp.einsum('hqj,jhe->qhe', own_weight.astype(jnp.float32), value_new.astype(jnp.float32))
        return lax.optimization_barrier(jnp.sum(partial_value, axis=0)) + own_term
    attended = lax.map(one_sequence, (queries, new_keys, new_values, key_cache, value_cache, starts, visible))
    mixed_out = attended * lax.rsqrt(lax.optimization_barrier(jnp.mean(attended * attended, axis=-1, keepdims=True)) + 1e-05)
    mixed_out = (mixed_out * sub_gain.astype(jnp.float32) * LAMBDA_SCALE).astype(jnp.bfloat16)
    mixed_out = mixed_out.reshape(batch_size * prop_count, head_count * 2 * head_dim)
    group_cols = head_count * 2 * head_dim // N_TP
    totals_out = jnp.zeros((batch_size * prop_count, width_all), jnp.float32)
    for member in range(N_TP):
        product = jnp.dot(mixed_out[:, member * group_cols:(member + 1) * group_cols], out_weight[member * group_cols:(member + 1) * group_cols], preferred_element_type=jnp.float32)
        totals_out = totals_out + lax.optimization_barrier(product.astype(jnp.bfloat16)).astype(jnp.float32)
    output = totals_out.astype(jnp.bfloat16).reshape(batch_size, prop_count, width_all)
    return (output, key_out, value_out)
```

```python
import math

import jax
import jax.numpy as jnp
from jax import lax
from jax.sharding import PartitionSpec as P

LAMBDA_SCALE = 0.2 + 0.6 * math.exp(-0.6)
NEG_FILL = -1e30
F32 = jnp.float32
BF16 = jnp.bfloat16


def grid_of(kv):
    inner = 1
    while kv % (inner * 2) == 0 and (inner * 2) ** 2 <= kv:
        inner *= 2
    return kv // inner, inner


def visible_links(parents):
    number = parents.shape[-1]
    identity = jnp.eye(number, dtype=F32)
    links = (parents[..., :, None] == jnp.arange(number, dtype=jnp.int32)).astype(F32)
    reached = jnp.maximum(links, identity)
    span = 1
    while span < number:
        reached = jnp.minimum(
            jnp.einsum("bij,bjk->bik", reached.astype(BF16), reached.astype(BF16), preferred_element_type=F32), 1.0
        )
        span *= 2
    depths = (jnp.sum(reached, axis=-1) - 1.0).astype(jnp.int32)
    return reached > 0.5, depths


def turn_table(positions, half_dim):
    frequency = 10000.0 ** (-jnp.arange(half_dim, dtype=F32) / half_dim)
    angles = positions.astype(F32)[..., None] * frequency
    return jnp.cos(angles), jnp.sin(angles)


def rotate(values, table):
    cosine, sine = (part[:, None, None, :] for part in table)
    half_dim = values.shape[-1] // 2
    low = values[..., :half_dim]
    high = values[..., half_dim:]
    return jnp.concatenate([low * cosine - high * sine, high * cosine + low * sine], axis=-1)


def merge_stats(former, latter):
    highest = jnp.maximum(former[0], latter[0])
    totals = former[1] * jnp.exp(former[0] - highest) + latter[1] * jnp.exp(latter[0] - highest)
    return (highest, totals)


def make_body(kv, tp):
    Z, Y = grid_of(kv)

    def body(
        tokens, in_gain, query_weight, key_weight, value_weight, out_weight, lambdas, sub_gain,
        key_cache, value_cache, cache_len, accepted, parents,
    ):
        seqs, props, width = tokens.shape
        heads = lambdas.shape[0]
        span = key_cache.shape[1]
        hd = key_cache.shape[-1]
        Sy = seqs // Y
        Ry = Sy * props
        Hz = heads // Z
        cz = Hz * 2 * hd
        width_all = width * kv
        k = lax.axis_index("kv")
        y = k % Y
        z = k // Y

        def yperm(x, s):
            return lax.ppermute(x, "kv", [(i, (i // Y) * Y + ((i % Y) ^ s)) for i in range(kv)])

        def zperm(x, s):
            return lax.ppermute(x, "kv", [(i, ((i // Y) ^ s) * Y + i % Y) for i in range(kv)])

        def natural(parts, index):
            parts = list(parts)
            bit = 1
            while bit < len(parts):
                odd = (index & bit) != 0
                parts = [jnp.where(odd, parts[s ^ bit], parts[s]) for s in range(len(parts))]
                bit *= 2
            return parts

        def yrows(a, which):
            size = a.shape[0] // Y
            return lax.dynamic_slice_in_dim(a, which * size, size, 0)

        def zcols(a, which):
            return lax.dynamic_slice_in_dim(a, which * cz, cz, 1)

        wide = tokens.astype(F32)
        normed = (wide * in_gain.astype(F32)).astype(BF16).reshape(seqs * props, width)
        squares = jnp.sum(wide * wide, axis=-1).reshape(seqs * props)

        def send_y(weight):
            return [
                yperm(jnp.dot(yrows(normed, y ^ s), weight, preferred_element_type=F32).astype(BF16), s)
                for s in range(1, Y)
            ]

        def sum_y(weight, got):
            total = jnp.dot(yrows(normed, y), weight, preferred_element_type=F32)
            for part in got:
                total = total + part.astype(F32)
            return total

        def send_z(total):
            return [zperm(zcols(total, z ^ s).astype(BF16), s) for s in range(1, Z)]

        def sum_z(total, got):
            total = zcols(total, z)
            for part in got:
                total = total + part.astype(F32)
            return total

        got_q = send_y(query_weight)
        sq = yrows(squares, y)
        for part in [yperm(yrows(squares, y ^ s), s) for s in range(1, Y)]:
            sq = sq + part
        for part in [zperm(sq, s) for s in range(1, Z)]:
            sq = sq + part
        row_scale = lax.rsqrt(sq / width_all + 1e-06)[:, None]

        sum_q = sum_y(query_weight, got_q)
        got_qz = send_z(sum_q)
        got_k = send_y(key_weight)
        sum_k = sum_y(key_weight, got_k)
        got_kz = send_z(sum_k)
        got_v = send_y(value_weight)
        sum_v = sum_y(value_weight, got_v)
        got_vz = send_z(sum_v)

        starts_all = cache_len + accepted
        starts = yrows(starts_all, y)
        visible, depths = visible_links(yrows(parents, y))
        table = turn_table((starts[:, None] + depths).reshape(Ry), hd // 2)

        vec = (Ry, Hz, 2, hd)
        q_own = rotate((sum_z(sum_q, got_qz) * row_scale).reshape(vec), table).astype(BF16).reshape(Ry, cz)
        q_all = natural([q_own] + [zperm(q_own, s) for s in range(1, Z)], z)
        q_all = jnp.stack(q_all).reshape(Z, Sy, props, Hz, 2, hd)
        k_own = rotate((sum_z(sum_k, got_kz) * row_scale).reshape(vec), table).astype(BF16).reshape(Ry, cz)
        v_own = (sum_z(sum_v, got_vz) * row_scale).astype(BF16)

        def cache_y(cache):
            parts = [yrows(cache, y)] + [yperm(yrows(cache, y ^ s), s) for s in range(1, Y)]
            return jnp.stack(parts, axis=1)

        keys = cache_y(key_cache).reshape(Sy, Y * span, Z, Hz, 2, hd)
        values = cache_y(value_cache).reshape(Sy, Y * span, Z, Hz, 2 * hd)
        order = jnp.stack([z * Y + (y ^ s) for s in range(Y)])
        spots = (order[:, None] * span + jnp.arange(span, dtype=jnp.int32)).reshape(Y * span)
        live = (spots[None, :] < starts[:, None])[None, :, None, None, None, :]

        inverse_root = hd ** (-0.5)
        scores = (
            jnp.einsum("zbqhmd,btzhmd->zbhmqt", q_all, keys, preferred_element_type=F32) * inverse_root
        )
        scores = jnp.where(live, scores, NEG_FILL)
        local_peak = jnp.max(scores, axis=-1)
        local_total = jnp.sum(jnp.where(live, jnp.exp(scores - local_peak[..., None]), 0.0), axis=-1)

        q_b = q_own.reshape(Sy, props, Hz, 2, hd)
        k_b = k_own.reshape(Sy, props, Hz, 2, hd)
        v_b = v_own.reshape(Sy, props, Hz, 2 * hd)
        own_scores = jnp.einsum("bqhmd,bjhmd->bhmqj", q_b, k_b, preferred_element_type=F32) * inverse_root
        seen = visible[:, None, None]
        own_scores = jnp.where(seen, own_scores, NEG_FILL)
        own_peak = jnp.max(own_scores, axis=-1)
        own_total = jnp.sum(jnp.where(seen, jnp.exp(own_scores - own_peak[..., None]), 0.0), axis=-1)

        mine = jnp.stack([local_peak, local_total])
        own_stats = jnp.stack([own_peak, own_total])
        packed = jnp.concatenate([mine, own_stats[:, None]], axis=1)
        got = [packed] + [zperm(packed, s) for s in range(1, Z)]
        stat = (mine[0], mine[1])
        for part in got[1:]:
            stat = merge_stats(stat, (part[0, :Z], part[1, :Z]))
        own_all = jnp.stack(natural([part[:, Z] for part in got], z))
        peak_all, totals = merge_stats(stat, (own_all[:, 0], own_all[:, 1]))

        def at_z(a, which):
            return lax.dynamic_index_in_dim(a, which, 0, keepdims=False)

        lam = lambdas.reshape(Z, Hz)

        def weights_of(scores, alive, peak, total, lam_mix):
            probs = jnp.where(alive, jnp.exp(scores - peak[..., None]), 0.0) / total[..., None]
            return (probs[..., 0, :, :] - lam_mix * probs[..., 1, :, :]).astype(BF16)

        cache_weight = weights_of(scores, live, peak_all, totals, lam[:, None, :, None, None])
        partial = jnp.einsum("zbhqt,btzhe->zbqhe", cache_weight, values, preferred_element_type=F32)
        attended = at_z(partial, z).astype(BF16).astype(F32)
        for part in [zperm(at_z(partial, z ^ s).astype(BF16), s) for s in range(1, Z)]:
            attended = attended + part.astype(F32)
        own_weight = weights_of(
            own_scores, seen, at_z(peak_all, z), at_z(totals, z), at_z(lam, z)[None, :, None, None]
        )
        attended = attended + jnp.einsum("bhqj,bjhe->bqhe", own_weight, v_b, preferred_element_type=F32)
        mixed = attended * lax.rsqrt(jnp.mean(attended * attended, axis=-1, keepdims=True) + 1e-05)
        mixed = (mixed * sub_gain.astype(F32) * LAMBDA_SCALE).astype(BF16).reshape(Ry, cz)

        def spread(chunk):
            whole = jnp.concatenate(natural([chunk] + [zperm(chunk, s) for s in range(1, Z)], z), axis=-1)
            return [whole] + [yperm(whole, s) for s in range(1, Y)]

        products = [
            jnp.dot(rows, out_weight, preferred_element_type=F32).astype(BF16) for rows in spread(mixed)
        ]
        product = jnp.concatenate(natural(products, y), axis=0).reshape(seqs, props, -1)
        share = product.shape[-1] // tp
        t = lax.axis_index("tp")

        def tcols(which):
            return lax.dynamic_slice_in_dim(product, which * share, share, 2)

        output = tcols(t).astype(F32)
        for s in range(1, tp):
            output = output + lax.ppermute(
                tcols(t ^ s), "tp", [(i, i ^ s) for i in range(tp)]
            ).astype(F32)
        output = output.astype(BF16)

        kv_new = jnp.stack([k_own, v_own])
        new_all = jnp.concatenate(natural(spread(kv_new), y), axis=1)
        offset = k * span
        slot = offset + jnp.arange(span, dtype=jnp.int32)[None, :] - starts_all[:, None]
        pick = (slot[:, :, None] == jnp.arange(props, dtype=jnp.int32)).astype(BF16)
        fresh = (slot >= 0) & (slot < props)
        new_all = new_all.reshape(2, seqs, props, heads * 2 * hd)

        def written(cache, new):
            moved = jnp.einsum("btj,bje->bte", pick, new, preferred_element_type=F32).astype(BF16)
            flat = moved.reshape(cache.shape)
            mask = fresh.reshape(fresh.shape + (1,) * (cache.ndim - 2))
            return jnp.where(mask, flat, cache)

        return (output, written(key_cache, new_all[0]), written(value_cache, new_all[1]))

    return body


def solution(mesh):
    placed = (
        P("dp", None, "kv"),
        P("kv"),
        P("kv", "tp"),
        P("kv", "tp"),
        P("kv", "tp"),
        P("tp", "kv"),
        P("tp"),
        P(),
        P("dp", "kv", "tp", None, None),
        P("dp", "kv", "tp", None),
        P("dp"),
        P("dp"),
        P("dp", None),
    )
    return jax.shard_map(
        make_body(mesh.shape["kv"], mesh.shape["tp"]),
        mesh=mesh,
        in_specs=placed,
        out_specs=(
            P("dp", None, ("kv", "tp")),
            P("dp", "kv", "tp", None, None),
            P("dp", "kv", "tp", None),
        ),
        check_vma=False,
    )
```
